32 devices in a mesh: grp: 2 (over x), sp: 8 (over z, y), tp: 2 (over core).
Axes of the slice: x: 2, y: 2, z: 4, core: 2. Of those that a mesh axis runs over, the one named last changes fastest.
Arguments:
- tokens: bfloat16 [8192, 2048], P(('grp', 'sp', 'tp')), parts along dimension 0, may hold values from -8 to 8
- in_gain: float32 [2048], replicated, may hold values from 0.1 to 1.9
- w_query: bfloat16 [2048, 1024], P(None, 'tp'), may hold values from -0.125 to 0.125
- w_forget: bfloat16 [2048, 1024], P(None, 'tp'), may hold values from -0.125 to 0.125
- w_value: bfloat16 [2048, 1024], P(None, 'tp'), may hold values from -1 to 1
- w_outgate: bfloat16 [2048, 1024], P(None, 'tp'), may hold values from -0.125 to 0.125
- floor_gap: float32 [1024], P('tp'), may hold values from 0 to 0.1, as said below
- extra_decay: float32 [8192, 8], P(('grp', 'sp'), 'tp'), parts along dimension 0, may hold values from -3 to 0
- out_gain: bfloat16 [1024], P('tp'), may hold values from 0.099609375 to 1.8984375
- w_output: bfloat16 [1024, 2048], P('tp'), may hold values from -0.1875 to 0.1875
Outputs:
- mixed_out: bfloat16 [8192, 2048], P(('grp', 'sp', 'tp')), parts along dimension 0
The draws below stay inside these ranges and needn't reach their ends.
There are 2 independent parts, one for each index of `grp`. The reference program is written for one: setup_inputs(seed, part) draws one part's arguments, and reference() takes and returns one part's arrays. A program takes and returns all parts, laid end to end along the dimension named above; an argument that names none is the same for every part. Nothing has to cross between parts.
Inputs may be any that keep to these rules, and one draw needn't show every extreme that they name: `floor_gap`: every entry is positive.
All inputs are finite; a program needn't handle non-finite values.
Results may differ from the reference program's by a relative error of at most 0.015.
Values may be sent and summed in bfloat16 or wider, within the bound.
A program may use at most 128 MiB of HBM per device.

```python
import jax
import jax.numpy as jnp
from jax import lax

D = 2048
LOOP_GROUPS = 8
HEAD_K = 128
HEAD_V = 128
BLOCK = 32
TOK_DEV = 256
KWIDTH = 1024
VWIDTH = 1024
TOKEN_COUNT = 4096
N_SP = 8
N_TP = 2


def draw_tokens(key, part):
    first, right_factor, extra_factor = jax.random.split(key, 3)
    mean_dir = jax.random.normal(first, (D,), jnp.float32)
    block_scale = jax.random.uniform(right_factor, (N_SP * N_TP,), jnp.float32, 0.3, 1.5)
    owner = (jnp.arange(TOKEN_COUNT) // TOK_DEV).astype(jnp.int32)
    noise = jax.random.normal(extra_factor, (TOKEN_COUNT, D), jnp.float32)
    returned_value = jnp.clip(mean_dir[None, :] * block_scale[owner][:, None] + noise, -8.0, 8.0)
    return returned_value.astype(jnp.bfloat16)


def draw_w_value(key, part):
    first, right_factor = jax.random.split(key, 2)
    base = jax.random.normal(first, (D, VWIDTH), jnp.float32)
    head_index = (jnp.arange(VWIDTH) // HEAD_V).astype(jnp.float32)
    rising = 1.0 + 2.0 * head_index / max(LOOP_GROUPS - 1, 1)
    column = jnp.exp(jax.random.uniform(right_factor, (VWIDTH,), jnp.float32, jnp.log(0.7), jnp.log(1.4)))
    returned_value = jnp.clip(base * D ** (-0.5) * (rising * column)[None, :], -1.0, 1.0)
    return returned_value.astype(jnp.bfloat16)


def draw_floor_gap(key, part):
    first, right_factor, extra_factor = jax.random.split(key, 3)
    fast_share = 0.5
    fast_heads = jax.random.uniform(first, (LOOP_GROUPS,), jnp.float32) < fast_share
    fast_gap = jnp.exp(jax.random.uniform(right_factor, (KWIDTH,), jnp.float32, jnp.log(0.03), jnp.log(0.1)))
    slow_low = jnp.log(jnp.float32(0.3 / TOKEN_COUNT))
    slow_high = jnp.log(jnp.float32(1.5 / TOK_DEV))
    slow_gap = jnp.exp(jax.random.uniform(extra_factor, (KWIDTH,), jnp.float32, slow_low, slow_high))
    head_index = (jnp.arange(KWIDTH) // HEAD_K).astype(jnp.int32)
    return jnp.where(fast_heads[head_index], fast_gap, slow_gap).astype(jnp.float32)


def draw_extra_decay(key, part):
    first, right_factor, extra_factor = jax.random.split(key, 3)
    upper = 2.0
    factor = jnp.exp(jax.random.uniform(first, (N_SP, LOOP_GROUPS), jnp.float32, jnp.log(0.5), jnp.log(upper)))
    owner = (jnp.arange(TOKEN_COUNT) // (TOKEN_COUNT // N_SP)).astype(jnp.int32)
    returned_value = -factor[owner] * (0.3 / TOKEN_COUNT)
    span_start = jax.random.randint(right_factor, (3, LOOP_GROUPS), 0, TOKEN_COUNT)
    span_size = jax.random.uniform(extra_factor, (3, LOOP_GROUPS), jnp.float32, jnp.log(0.5), jnp.log(0.8))
    destination_slots = jnp.arange(TOKEN_COUNT).astype(jnp.int32)[:, None]
    for token_slot in range(3):
        returned_value = returned_value + jnp.where(destination_slots == span_start[token_slot][None, :], span_size[token_slot][None, :], 0.0)
    return returned_value.astype(jnp.float32)


def level_of(own_key, extent, pieces, least, high):
    loudness = 1.0
    for position, parts in pieces:
        heights = jax.random.uniform(jax.random.fold_in(jax.random.fold_in(own_key, 6), position), (parts,), jnp.float32, least / len(pieces), high / len(pieces))
        loudness = loudness * jnp.repeat(jnp.exp(heights), extent[position] // parts).reshape((-1,) + (1,) * (len(extent) - 1 - position))
    return loudness


def bell_draw(stream_key, dims, width, limit, pieces=(), kind=jnp.bfloat16):
    drawn = jax.random.normal(stream_key, dims, jnp.float32) * width
    if len(pieces) > 0:
        drawn = level_of(stream_key, dims, pieces, -0.22, 0.18) * drawn
    return jnp.clip(drawn, min=-limit, max=limit).astype(kind)


def setup_inputs(seed: int = 0, part: int = 0) -> dict:
    streams_of = jax.random.split(jax.random.key(seed), 11)
    part_splits = jax.random.split(jax.random.fold_in(streams_of[10], part), 11)
    tokens = draw_tokens(jax.random.fold_in(jax.random.fold_in(streams_of[10], part), 71), part)
    in_gain = jnp.clip(1.0 + 0.18 * jax.random.normal(streams_of[1], (D,), jnp.float32), 0.1, 1.9)
    w_query = bell_draw(streams_of[2], (D, KWIDTH), D ** -0.5, 0.125, ((1, 2),))
    w_forget = bell_draw(streams_of[3], (D, KWIDTH), D ** -0.5, 0.125, ((1, 2),))
    w_value = draw_w_value(jax.random.fold_in(streams_of[10], 71), part)
    w_outgate = bell_draw(streams_of[5], (D, VWIDTH), D ** -0.5, 0.125, ((1, 2),))
    floor_gap = draw_floor_gap(jax.random.fold_in(streams_of[10], 71), part)
    extra_decay = draw_extra_decay(jax.random.fold_in(jax.random.fold_in(streams_of[10], part), 71), part)
    out_gain = jnp.clip(1.0 + 0.18 * jax.random.normal(streams_of[8], (VWIDTH,), jnp.float32), 0.099609375, 1.8984375).astype(jnp.bfloat16)
    w_output = bell_draw(streams_of[9], (VWIDTH, D), VWIDTH ** -0.5, 0.1875, ((0, 2),))
    return {"tokens": tokens, "in_gain": in_gain, "w_query": w_query, "w_forget": w_forget, "w_value": w_value, "w_outgate": w_outgate, "floor_gap": floor_gap, "extra_decay": extra_decay, "out_gain": out_gain, "w_output": w_output}


epsilon = 1e-06
highest = lax.Precision.HIGHEST

def gate_terms(query_proj, forget_pre, value_proj, floor_gap, extra_decay):
    tok_rows = query_proj.shape[0]
    head_count = floor_gap.shape[0] // HEAD_K
    reading = jax.nn.silu(query_proj.astype(jnp.float32)).reshape(tok_rows, head_count, HEAD_K) * HEAD_K ** (-0.5)
    pre_gate = forget_pre.astype(jnp.float32).reshape(tok_rows, head_count, HEAD_K)
    floor_part = floor_gap.reshape(head_count, HEAD_K)
    key_terms = floor_part * jax.nn.sigmoid(-pre_gate)
    log_forget = jnp.logaddexp(jnp.log1p(-floor_part), jnp.log(floor_part) + jax.nn.log_sigmoid(pre_gate))
    log_forget = log_forget + extra_decay[:, :, None]
    values = value_proj.astype(jnp.float32).reshape(tok_rows, head_count, HEAD_V)
    return (reading, key_terms, values, log_forget)

def blockwise(reading, key_terms, values, log_forget):
    positions, head_count, key_width = reading.shape
    value_width = values.shape[-1]
    block_count = positions // BLOCK

    def to_blocks(tensor):
        return tensor.reshape(block_count, BLOCK, head_count, tensor.shape[-1]).transpose(0, 2, 1, 3)

    def from_blocks(tensor):
        return tensor.transpose(0, 2, 1, 3).reshape(positions, head_count, tensor.shape[-1])
    causal_mask = jnp.tril(jnp.ones((BLOCK, BLOCK), dtype=bool))[:, :, None]

    def advance(carried, inputs):
        carry_state, offset = carried
        read_block, key_block, value_block, gate_block = inputs
        cumulative = jnp.cumsum(gate_block, axis=1)
        across = jnp.einsum('hid,hde->hie', read_block * jnp.exp(cumulative), carry_state, precision=highest)
        differ = cumulative[:, :, None, :] - cumulative[:, None, :, :]
        decays = jnp.exp(jnp.where(causal_mask, differ, -jnp.inf))
        scores = jnp.einsum('hid,hjd,hijd->hij', read_block, key_block, decays, precision=highest)
        within = jnp.einsum('hij,hje->hie', scores, value_block, precision=highest)
        last_sum = cumulative[:, -1:, :]
        weighted = key_block * jnp.exp(last_sum - cumulative)
        carry_state = jnp.exp(last_sum[:, 0, :, None]) * carry_state + jnp.einsum('hjd,hje->hde', weighted, value_block, precision=highest)
        return ((carry_state, offset + last_sum[:, 0, :]), (across + within, cumulative + offset[:, None, :]))
    start_state = jnp.zeros((head_count, key_width, value_width), jnp.float32)
    start_offset = jnp.zeros((head_count, key_width), jnp.float32)
    ended, produced = lax.scan(advance, (start_state, start_offset), (to_blocks(reading), to_blocks(key_terms), to_blocks(values), to_blocks(log_forget)))
    return (from_blocks(produced[0]), from_blocks(produced[1]), ended[0], ended[1])

def reference(tokens, in_gain, w_query, w_forget, w_value, w_outgate, floor_gap, extra_decay, out_gain, w_output):
    widened = tokens.astype(jnp.float32)
    normed = (widened * lax.rsqrt(lax.optimization_barrier(jnp.mean(widened * widened, axis=-1, keepdims=True)) + epsilon) * in_gain).astype(jnp.bfloat16)
    query_proj = jnp.dot(normed, w_query, preferred_element_type=jnp.float32).astype(jnp.bfloat16)
    forget_pre = jnp.dot(normed, w_forget, preferred_element_type=jnp.float32).astype(jnp.bfloat16)
    value_proj = jnp.dot(normed, w_value, preferred_element_type=jnp.float32).astype(jnp.bfloat16)
    out_gate = jnp.dot(normed, w_outgate, preferred_element_type=jnp.float32).astype(jnp.bfloat16)
    reading, key_terms, values, log_forget = gate_terms(query_proj, forget_pre, value_proj, floor_gap, extra_decay)
    outputs, running, end_state, end_offset = blockwise(reading, key_terms, values, log_forget)
    tok_rows = outputs.shape[0]
    recur_out = outputs.astype(jnp.bfloat16).reshape(tok_rows, outputs.shape[1] * outputs.shape[2])
    recur_wide = recur_out.astype(jnp.float32)
    inv_scale = lax.rsqrt(lax.optimization_barrier(jnp.mean(recur_wide * recur_wide, axis=-1, keepdims=True)) + epsilon)
    gated = (recur_wide * inv_scale * out_gain.astype(jnp.float32) * jax.nn.silu(out_gate.astype(jnp.float32))).astype(jnp.bfloat16)
    return jnp.dot(gated, w_output, preferred_element_type=jnp.float32).astype(jnp.bfloat16)
```

```python
import functools

import jax
import jax.numpy as jnp
from jax import lax
from jax.experimental import pallas as pl
from jax.experimental.pallas import tpu as pltpu
from jax.sharding import PartitionSpec as P

HEAD = 128
CHUNK = 128
MESH = pl.DeviceIdType.MESH
epsilon = 1e-06
f32 = jnp.float32
bf16 = jnp.bfloat16


def dot(a, b):
    return jnp.dot(a, b, preferred_element_type=f32)


def dot_nt(a, b):
    return lax.dot_general(a, b, (((1,), (1,)), ((), ())), preferred_element_type=f32)


def dot_tn(a, b):
    return lax.dot_general(a, b, (((0,), (0,)), ((), ())), preferred_element_type=f32)


def split(x, parts):
    pieces = []
    for _ in range(parts):
        piece = x.astype(bf16)
        pieces.append(piece)
        x = x - piece.astype(f32)
    return pieces


def kernel(
    pairs,
    tokens, in_gain, w_query, w_forget, w_value, w_outgate, floor_gap, extra, out_gain, w_output,
    out,
    tok, normed, weights, wo, proj, cum_gate, cum_extra, key_up, read_down, local_out,
    starts, offsets, own_state, own_decay, end_bf, peer_bf, peer_decay, chain_in, chain_out, incoming,
    gate_send, gate_recv, square_send, square_recv, gate_own, partial,
    load_sem, wide_send, wide_recv, state_send, state_recv, chain_send, chain_recv, last_send, last_recv,
):
    half, width = tok.shape[1], tok.shape[2]
    rows = 2 * half
    chans = floor_gap.shape[1]
    heads = chans // HEAD
    chunks = rows // CHUNK
    me = lax.axis_index("tp")
    other = 1 - me
    place = lax.axis_index("sp")
    side = place % 2
    link = place // 2
    mate = place + 1 - 2 * side

    loads = [pltpu.make_async_copy(tokens, tok.at[0], load_sem.at[0])]
    order = (w_forget, w_value, w_query, w_outgate)
    for n, w in enumerate(order):
        loads.append(pltpu.make_async_copy(w, weights.at[n], load_sem.at[1 + n]))
    loads.append(pltpu.make_async_copy(w_output, wo.at[0], load_sem.at[5]))
    for copy in loads:
        copy.start()

    barrier = pltpu.get_barrier_semaphore()
    pl.semaphore_signal(barrier, inc=1, device_id={"tp": other}, device_id_type=MESH)
    pl.semaphore_signal(barrier, inc=1, device_id={"sp": mate}, device_id_type=MESH)

    @pl.when(link > 0)
    def _():
        pl.semaphore_signal(barrier, inc=1, device_id={"sp": place - 2}, device_id_type=MESH)

    @pl.when(link < pairs - 1)
    def _():
        pl.semaphore_signal(barrier, inc=1, device_id={"sp": place + 2}, device_id_type=MESH)

    peers = 2 + jnp.minimum(link, 1) + jnp.minimum(pairs - 1 - link, 1)
    pl.semaphore_wait(barrier, peers)

    def to_tp(src, dst, send, recv):
        return pltpu.make_async_remote_copy(
            src_ref=src, dst_ref=dst, send_sem=send, recv_sem=recv,
            device_id={"tp": other}, device_id_type=MESH,
        )

    def to_sp(src, dst, send, recv, target):
        return pltpu.make_async_remote_copy(
            src_ref=src, dst_ref=dst, send_sem=send, recv_sem=recv,
            device_id={"sp": target}, device_id_type=MESH,
        )

    tok_copy = to_tp(tokens, tok.at[1], wide_send.at[0], wide_recv.at[0])
    tok_copy.start()
    wo_copy = to_tp(w_output, wo.at[1], wide_send.at[1], wide_recv.at[1])

    def normalize(slot, base):
        step = 64

        def block(n, _):
            x = tok[slot, pl.ds(pl.multiple_of(n * step, step), step), :].astype(f32)
            inv = lax.rsqrt(jnp.mean(x * x, axis=-1, keepdims=True) + epsilon)
            normed[pl.ds(pl.multiple_of(base + n * step, step), step), :] = (
                x * inv * in_gain[...]
            ).astype(bf16)
            return 0

        lax.fori_loop(0, half // step, block, 0)

    loads[0].wait()
    normalize(0, me * half)
    tok_copy.wait_recv()
    wo_copy.start()
    normalize(1, other * half)

    def project(n):
        loads[1 + n].wait()
        step = 256

        def block(k, _):
            cols = pl.ds(pl.multiple_of(k * step, step), step)
            proj[n, :, cols] = dot(normed[...], weights[n, :, cols]).astype(bf16)
            return 0

        lax.fori_loop(0, chans // step, block, 0)

    project(0)
    project(1)

    later = lax.broadcasted_iota(jnp.int32, (CHUNK, CHUNK), 0)
    sooner = lax.broadcasted_iota(jnp.int32, (CHUNK, CHUNK), 1)
    mask = later >= sooner
    lower = jnp.where(mask, 1.0, 0.0).astype(bf16)

    own_state[...] = jnp.zeros_like(own_state)
    own_decay[...] = jnp.zeros_like(own_decay)

    def states(c, _):
        at = pl.ds(pl.multiple_of(c * CHUNK, CHUNK), CHUNK)
        key = floor_gap[...] / (1.0 + jnp.exp(proj[0, at, :].astype(f32)))
        gate = jnp.log1p(-key)
        summed = sum(dot(lower, piece) for piece in split(gate, 2))
        here = extra[at, :]
        wide = jnp.concatenate(
            [jnp.broadcast_to(here[:, h : h + 1], (CHUNK, HEAD)) for h in range(heads)], axis=1
        )
        extra_sum = sum(dot(lower, piece) for piece in split(wide, 3))
        cum_gate[at, :] = summed
        cum_extra[at, :] = extra_sum
        key_up[at, :] = (key * jnp.exp(-summed)).astype(bf16)
        both = summed + extra_sum
        last = both[CHUNK - 1 : CHUNK, :]
        kept = (key * jnp.exp(last - both)).astype(bf16)
        shrink = jnp.exp(last)
        offsets[c] = own_decay[0:1, :]
        own_decay[...] = own_decay[...] + last
        for h in range(heads):
            cols = slice(h * HEAD, (h + 1) * HEAD)
            state = own_state[h]
            starts[c, h] = state.astype(bf16)
            own_state[h] = state * shrink[:, cols] + dot_tn(proj[1, at, cols], kept[:, cols])
        return 0

    lax.fori_loop(0, chunks, states, 0)
    end_bf[...] = own_state[...].astype(bf16)

    decay_copy = to_sp(own_decay, peer_decay, state_send.at[heads], state_recv.at[heads], mate)
    decay_copy.start()
    state_copies = []
    for h in range(heads):
        copy = to_sp(end_bf.at[h], peer_bf.at[h], state_send.at[h], state_recv.at[h], mate)
        copy.start()
        state_copies.append(copy)

    project(2)
    project(3)

    def outputs(c, _):
        at = pl.ds(pl.multiple_of(c * CHUNK, CHUNK), CHUNK)
        query = proj[2, at, :].astype(f32)
        reading = query / (1.0 + jnp.exp(-query)) * HEAD ** (-0.5)
        extra_sum = cum_extra[at, :]
        near = reading * jnp.exp(cum_gate[at, :])
        far = near * jnp.exp(extra_sum)
        read_down[at, :] = (far * jnp.exp(offsets[c])).astype(bf16)
        near = near.astype(bf16)
        far = far.astype(bf16)
        for h in range(heads):
            cols = slice(h * HEAD, (h + 1) * HEAD)
            scores = dot_nt(near[:, cols], key_up[at, cols])
            column = extra_sum[:, cols]
            decay = jnp.where(mask, jnp.exp(column - column.T), 0.0)
            local_out[at, cols] = dot((scores * decay).astype(bf16), proj[1, at, cols]) + dot_nt(
                far[:, cols], starts[c, h]
            )
        return 0

    def compute_outputs():
        lax.fori_loop(0, chunks, outputs, 0)

    onward = [
        to_sp(chain_out.at[h], chain_in.at[h], chain_send.at[h], chain_recv.at[h], place + 2)
        for h in range(heads)
    ]
    second = side.astype(f32)
    first = 1.0 - second

    def relay():
        decay_copy.wait_recv()
        mine = own_decay[0:1, :]
        theirs = peer_decay[0:1, :]
        early = first * mine + second * theirs
        late = first * theirs + second * mine

        @pl.when(link == 0)
        def _():
            chain_in[...] = jnp.zeros_like(chain_in)

        for h in range(heads):
            cols = slice(h * HEAD, (h + 1) * HEAD)
            state_copies[h].wait_recv()

            @pl.when(link > 0)
            def _():
                onward[h].wait_recv()

            own = own_state[h]
            peer = peer_bf[h].astype(f32)
            begun = first * own + second * peer
            ended = first * peer + second * own
            before = chain_in[h].astype(f32)
            middle = jnp.exp(early[:, cols]) * before + begun

            @pl.when(link < pairs - 1)
            def _():
                chain_out[h] = (jnp.exp(late[:, cols]) * middle + ended).astype(bf16)
                onward[h].start()

            incoming[h] = (first * before + second * middle).astype(bf16)

    front = pairs // 2

    @pl.when(link >= front)
    def _():
        compute_outputs()

    relay()

    @pl.when(link < front)
    def _():
        compute_outputs()

    def finish(base):
        at = pl.ds(pl.multiple_of(base, half), half)
        pieces = []
        squares = jnp.zeros((half, 1), f32)
        for h in range(heads):
            cols = slice(h * HEAD, (h + 1) * HEAD)
            total = local_out[at, cols] + dot_nt(read_down[at, cols], incoming[h])
            total = total.astype(bf16).astype(f32)
            squares = squares + jnp.sum(total * total, axis=-1, keepdims=True)
            gate = proj[3, at, cols].astype(f32)
            gated = total * out_gain[:, cols].astype(f32) * (gate / (1.0 + jnp.exp(-gate)))
            pieces.append(gated.astype(bf16))
        return pieces, squares

    pieces, squares = finish(other * half)
    for h in range(heads):
        gate_send[:, h * HEAD : (h + 1) * HEAD] = pieces[h]
    square_send[...] = jnp.broadcast_to(squares, square_send.shape)
    gate_copy = to_tp(gate_send, gate_recv, last_send.at[0], last_recv.at[0])
    square_copy = to_tp(square_send, square_recv, last_send.at[1], last_recv.at[1])
    gate_copy.start()
    square_copy.start()

    pieces, squares = finish(me * half)
    for h in range(heads):
        gate_own[:, h * HEAD : (h + 1) * HEAD] = pieces[h]
    tile = 512
    loads[5].wait()

    def own_part(k, _):
        cols = pl.ds(pl.multiple_of(k * tile, tile), tile)
        partial[:, cols] = dot(gate_own[...], wo[0, :, cols])
        return 0

    lax.fori_loop(0, width // tile, own_part, 0)
    wo_copy.wait_recv()
    gate_copy.wait_recv()
    square_copy.wait_recv()
    scale = lax.rsqrt((squares + square_recv[:, 0:1]) / (2.0 * chans) + epsilon)

    def whole(k, _):
        cols = pl.ds(pl.multiple_of(k * tile, tile), tile)
        both = partial[:, cols] + dot(gate_recv[...], wo[1, :, cols])
        out[:, cols] = (both * scale).astype(bf16)
        return 0

    lax.fori_loop(0, width // tile, whole, 0)

    tok_copy.wait_send()
    wo_copy.wait_send()
    decay_copy.wait_send()
    for copy in state_copies:
        copy.wait_send()

    @pl.when(link < pairs - 1)
    def _():
        for copy in onward:
            copy.wait_send()

    gate_copy.wait_send()
    square_copy.wait_send()


def body(
    tokens, in_gain, w_query, w_forget, w_value, w_outgate, floor_gap, extra_decay, out_gain, w_output
):
    half, width = tokens.shape
    rows = 2 * half
    chans = floor_gap.shape[0]
    heads = chans // HEAD
    chunks = rows // CHUNK
    vmem, sem = pltpu.VMEM, pltpu.SemaphoreType.DMA
    inner = pl.BlockSpec(memory_space=pltpu.VMEM)
    outer = pl.BlockSpec(memory_space=pl.ANY)
    square = (heads, HEAD, HEAD)
    return pl.pallas_call(
        functools.partial(kernel, lax.axis_size("sp") // 2),
        out_shape=jax.ShapeDtypeStruct((half, width), bf16),
        in_specs=[outer, inner, outer, outer, outer, outer, inner, inner, inner, outer],
        out_specs=inner,
        scratch_shapes=[
            vmem((2, half, width), bf16),
            vmem((rows, width), bf16),
            vmem((4, width, chans), bf16),
            vmem((2, chans, width), bf16),
            vmem((4, rows, chans), bf16),
            vmem((rows, chans), f32),
            vmem((rows, chans), f32),
            vmem((rows, chans), bf16),
            vmem((rows, chans), bf16),
            vmem((rows, chans), f32),
            vmem((chunks,) + square, bf16),
            vmem((chunks, 1, chans), f32),
            vmem(square, f32),
            vmem((8, chans), f32),
            vmem(square, bf16),
            vmem(square, bf16),
            vmem((8, chans), f32),
            vmem(square, bf16),
            vmem(square, bf16),
            vmem(square, bf16),
            vmem((half, chans), bf16),
            vmem((half, chans), bf16),
            vmem((half, HEAD), f32),
            vmem((half, HEAD), f32),
            vmem((half, chans), bf16),
            vmem((half, width), f32),
            sem((6,)),
            sem((2,)),
            sem((2,)),
            sem((heads + 1,)),
            sem((heads + 1,)),
            sem((heads,)),
            sem((heads,)),
            sem((2,)),
            sem((2,)),
        ],
        compiler_params=pltpu.CompilerParams(
            collective_id=0, has_side_effects=True, vmem_limit_bytes=56 * 1024 * 1024
        ),
    )(
        tokens, in_gain[None, :], w_query, w_forget, w_value, w_outgate,
        floor_gap[None, :], extra_decay, out_gain[None, :], w_output,
    )


def solution(mesh):
    in_specs = (
        P(("grp", "sp", "tp"), None),
        P(),
        P(None, "tp"),
        P(None, "tp"),
        P(None, "tp"),
        P(None, "tp"),
        P("tp"),
        P(("grp", "sp"), "tp"),
        P("tp"),
        P("tp", None),
    )
    out_specs = P(("grp", "sp", "tp"), None)
    return jax.shard_map(body, mesh=mesh, in_specs=in_specs, out_specs=out_specs, check_vma=False)
```

```python
import functools

import jax
import jax.numpy as jnp
from jax import lax
from jax.experimental import pallas as pl
from jax.experimental.pallas import tpu as pltpu
from jax.sharding import PartitionSpec as P

HEAD = 128
CHUNK = 128
PIECES = 2
MESH = pl.DeviceIdType.MESH
epsilon = 1e-06
f32 = jnp.float32
bf16 = jnp.bfloat16


def dot(a, b):
    return jnp.dot(a, b, preferred_element_type=f32)


def dot_nt(a, b):
    return lax.dot_general(a, b, (((1,), (1,)), ((), ())), preferred_element_type=f32)


def dot_tn(a, b):
    return lax.dot_general(a, b, (((0,), (0,)), ((), ())), preferred_element_type=f32)


def split(x, parts):
    pieces = []
    for _ in range(parts):
        piece = x.astype(bf16)
        pieces.append(piece)
        x = x - piece.astype(f32)
    return pieces


def kernel(
    pairs,
    tokens, in_gain_hbm, w_query, w_forget, w_value, w_outgate, floor_hbm, extra_hbm, out_gain_hbm, w_output,
    out,
    in_gain, floor_gap, extra, out_gain, tok, normed, weights, wo, proj, cum_gate, cum_extra, extra_line, key_up, read_down, local_out,
    starts, offsets, own_state, own_decay, end_bf, peer_bf, peer_decay, chain_in, chain_out, incoming,
    gate_send, gate_recv, square_send, square_recv, gate_own, partial,
    load_sem, wide_send, wide_recv, state_send, state_recv, chain_send, chain_recv, last_send, last_recv,
):
    half, width = tok.shape[1], tok.shape[2]
    rows = 2 * half
    chans = floor_gap.shape[1]
    heads = chans // HEAD
    chunks = rows // CHUNK
    me = lax.axis_index("tp")
    other = 1 - me
    place = lax.axis_index("sp")
    side = place % 2
    link = place // 2
    mate = place + 1 - 2 * side

    loads = [pltpu.make_async_copy(tokens, tok.at[0], load_sem.at[0])]
    order = (w_forget, w_value, w_query, w_outgate)
    for n, w in enumerate(order):
        loads.append(pltpu.make_async_copy(w, weights.at[n], load_sem.at[1 + n]))
    loads.append(pltpu.make_async_copy(w_output, wo.at[0], load_sem.at[5]))
    small = [
        pltpu.make_async_copy(src, dst, load_sem.at[6 + n])
        for n, (src, dst) in enumerate(
            ((in_gain_hbm, in_gain), (floor_hbm, floor_gap), (extra_hbm, extra), (out_gain_hbm, out_gain))
        )
    ]
    for copy in small + loads:
        copy.start()

    barrier = pltpu.get_barrier_semaphore()
    pl.semaphore_signal(barrier, inc=1, device_id={"tp": other}, device_id_type=MESH)
    pl.semaphore_signal(barrier, inc=1, device_id={"sp": mate}, device_id_type=MESH)

    @pl.when(link > 0)
    def _():
        pl.semaphore_signal(barrier, inc=1, device_id={"sp": place - 2}, device_id_type=MESH)

    @pl.when(link < pairs - 1)
    def _():
        pl.semaphore_signal(barrier, inc=1, device_id={"sp": place + 2}, device_id_type=MESH)

    peers = 2 + jnp.minimum(link, 1) + jnp.minimum(pairs - 1 - link, 1)
    pl.semaphore_wait(barrier, peers)

    def to_tp(src, dst, send, recv):
        return pltpu.make_async_remote_copy(
            src_ref=src, dst_ref=dst, send_sem=send, recv_sem=recv,
            device_id={"tp": other}, device_id_type=MESH,
        )

    def to_sp(src, dst, send, recv, target):
        return pltpu.make_async_remote_copy(
            src_ref=src, dst_ref=dst, send_sem=send, recv_sem=recv,
            device_id={"sp": target}, device_id_type=MESH,
        )

    tok_copy = to_tp(tokens, tok.at[1], wide_send.at[0], wide_recv.at[0])
    tok_copy.start()
    wo_copy = to_tp(w_output, wo.at[1], wide_send.at[1], wide_recv.at[1])

    def normalize(slot, base):
        step = 64

        def block(n, _):
            x = tok[slot, pl.ds(pl.multiple_of(n * step, step), step), :].astype(f32)
            inv = lax.rsqrt(jnp.mean(x * x, axis=-1, keepdims=True) + epsilon)
            normed[pl.ds(pl.multiple_of(base + n * step, step), step), :] = (
                x * inv * in_gain[...]
            ).astype(bf16)
            return 0

        lax.fori_loop(0, half // step, block, 0)

    for copy in small:
        copy.wait()
    def project(n, at):
        step = 256

        def block(k, _):
            cols = pl.ds(pl.multiple_of(k * step, step), step)
            proj[n, at, cols] = dot(normed[at, :], weights[n, :, cols]).astype(bf16)
            return 0

        lax.fori_loop(0, chans // step, block, 0)

    loads[0].wait()
    normalize(0, me * half)
    near_rows = pl.ds(pl.multiple_of(me * half, half), half)
    far_rows = pl.ds(pl.multiple_of(other * half, half), half)
    every = pl.ds(0, rows)
    loads[1].wait()
    project(0, near_rows)
    tok_copy.wait_recv()
    wo_copy.start()
    normalize(1, other * half)
    project(0, far_rows)
    loads[2].wait()
    project(1, every)

    later = lax.broadcasted_iota(jnp.int32, (CHUNK, CHUNK), 0)
    sooner = lax.broadcasted_iota(jnp.int32, (CHUNK, CHUNK), 1)
    mask = later >= sooner
    lower = jnp.where(mask, 1.0, 0.0).astype(bf16)
    upper = jnp.where(later <= sooner, 1.0, 0.0).astype(bf16)

    own_state[...] = jnp.zeros_like(own_state)
    own_decay[...] = jnp.zeros_like(own_decay)

    def states(c, _):
        at = pl.ds(pl.multiple_of(c * CHUNK, CHUNK), CHUNK)
        key = floor_gap[...] / (1.0 + jnp.exp(proj[0, at, :].astype(f32)))
        gate = jnp.log1p(-key)
        summed = sum(dot(lower, piece) for piece in split(gate, 2))
        line = sum(dot(piece, upper) for piece in split(extra[:, at], 3))
        extra_line[c] = line
        extra_sum = jnp.concatenate(
            [jnp.broadcast_to(line[h : h + 1, :], (HEAD, CHUNK)).T for h in range(heads)], axis=1
        )
        cum_gate[at, :] = summed
        cum_extra[at, :] = extra_sum
        key_up[at, :] = (key * jnp.exp(-summed)).astype(bf16)
        both = summed + extra_sum
        last = both[CHUNK - 1 : CHUNK, :]
        kept = (key * jnp.exp(last - both)).astype(bf16)
        shrink = jnp.exp(last)
        offsets[c] = own_decay[0:1, :]
        own_decay[...] = own_decay[...] + last
        for h in range(heads):
            cols = slice(h * HEAD, (h + 1) * HEAD)
            state = own_state[h]
            starts[c, h] = state.astype(bf16)
            own_state[h] = state * shrink[:, cols] + dot_tn(proj[1, at, cols], kept[:, cols])
        return 0

    lax.fori_loop(0, chunks, states, 0)
    end_bf[...] = own_state[...].astype(bf16)

    spans = [(h, pl.ds(p * (HEAD // PIECES), HEAD // PIECES)) for h in range(heads) for p in range(PIECES)]
    count = len(spans)
    decay_copy = to_sp(own_decay, peer_decay, state_send.at[count], state_recv.at[count], mate)
    decay_copy.start()
    state_copies = []
    for n, (h, span) in enumerate(spans):
        copy = to_sp(end_bf.at[h, span], peer_bf.at[h, span], state_send.at[n], state_recv.at[n], mate)
        copy.start()
        state_copies.append(copy)

    loads[3].wait()
    project(2, every)
    loads[4].wait()
    project(3, every)

    def outputs(c, _):
        at = pl.ds(pl.multiple_of(c * CHUNK, CHUNK), CHUNK)
        query = proj[2, at, :].astype(f32)
        reading = query / (1.0 + jnp.exp(-query)) * HEAD ** (-0.5)
        extra_sum = cum_extra[at, :]
        near = reading * jnp.exp(cum_gate[at, :])
        far = near * jnp.exp(extra_sum)
        read_down[at, :] = (far * jnp.exp(offsets[c])).astype(bf16)
        near = near.astype(bf16)
        far = far.astype(bf16)
        for h in range(heads):
            cols = slice(h * HEAD, (h + 1) * HEAD)
            scores = dot_nt(near[:, cols], key_up[at, cols])
            differ = extra_sum[:, cols] - extra_line[c, h : h + 1, :]
            decay = jnp.where(mask, jnp.exp(differ), 0.0)
            local_out[at, cols] = dot((scores * decay).astype(bf16), proj[1, at, cols]) + dot_nt(
                far[:, cols], starts[c, h]
            )
        return 0

    def compute_outputs():
        lax.fori_loop(0, chunks, outputs, 0)

    onward = [
        to_sp(chain_out.at[h, span], chain_in.at[h, span], chain_send.at[n], chain_recv.at[n], place + 2)
        for n, (h, span) in enumerate(spans)
    ]
    second = side.astype(f32)
    first = 1.0 - second

    def relay():
        decay_copy.wait_recv()
        mine = own_decay[0:1, :]
        theirs = peer_decay[0:1, :]
        early = first * mine + second * theirs
        late = first * theirs + second * mine

        @pl.when(link == 0)
        def _():
            chain_in[...] = jnp.zeros_like(chain_in)

        for n, (h, span) in enumerate(spans):
            cols = slice(h * HEAD, (h + 1) * HEAD)
            state_copies[n].wait_recv()

            @pl.when(link > 0)
            def _():
                onward[n].wait_recv()

            own = own_state[h, span]
            peer = peer_bf[h, span].astype(f32)
            begun = first * own + second * peer
            ended = first * peer + second * own
            before = chain_in[h, span].astype(f32)
            middle = jnp.exp(early[:, cols]) * before + begun

            @pl.when(link < pairs - 1)
            def _():
                chain_out[h, span] = (jnp.exp(late[:, cols]) * middle + ended).astype(bf16)
                onward[n].start()

            incoming[h, span] = (first * before + second * middle).astype(bf16)

    front = pairs // 2

    @pl.when(link >= front)
    def _():
        compute_outputs()

    relay()

    @pl.when(link < front)
    def _():
        compute_outputs()

    def finish(base):
        at = pl.ds(pl.multiple_of(base, half), half)
        pieces = []
        squares = jnp.zeros((half, 1), f32)
        for h in range(heads):
            cols = slice(h * HEAD, (h + 1) * HEAD)
            total = local_out[at, cols] + dot_nt(read_down[at, cols], incoming[h])
            total = total.astype(bf16).astype(f32)
            squares = squares + jnp.sum(total * total, axis=-1, keepdims=True)
            gate = proj[3, at, cols].astype(f32)
            gated = total * gains[:, cols] * (gate / (1.0 + jnp.exp(-gate)))
            pieces.append(gated.astype(bf16))
        return pieces, squares

    gains = out_gain[...].astype(f32).reshape(1, chans)

    pieces, squares = finish(other * half)
    for h in range(heads):
        gate_send[:, h * HEAD : (h + 1) * HEAD] = pieces[h]
    square_send[...] = jnp.broadcast_to(squares, square_send.shape)
    gate_copy = to_tp(gate_send, gate_recv, last_send.at[0], last_recv.at[0])
    square_copy = to_tp(square_send, square_recv, last_send.at[1], last_recv.at[1])
    gate_copy.start()
    square_copy.start()

    pieces, squares = finish(me * half)
    for h in range(heads):
        gate_own[:, h * HEAD : (h + 1) * HEAD] = pieces[h]
    tile = 512
    loads[5].wait()

    def own_part(k, _):
        cols = pl.ds(pl.multiple_of(k * tile, tile), tile)
        partial[:, cols] = dot(gate_own[...], wo[0, :, cols])
        return 0

    lax.fori_loop(0, width // tile, own_part, 0)
    wo_copy.wait_recv()
    gate_copy.wait_recv()
    square_copy.wait_recv()
    scale = lax.rsqrt((squares + square_recv[:, 0:1]) / (2.0 * chans) + epsilon)

    def whole(k, _):
        cols = pl.ds(pl.multiple_of(k * tile, tile), tile)
        both = partial[:, cols] + dot(gate_recv[...], wo[1, :, cols])
        out[:, cols] = (both * scale).astype(bf16)
        return 0

    lax.fori_loop(0, width // tile, whole, 0)

    tok_copy.wait_send()
    wo_copy.wait_send()
    decay_copy.wait_send()
    for copy in state_copies:
        copy.wait_send()

    @pl.when(link < pairs - 1)
    def _():
        for copy in onward:
            copy.wait_send()

    gate_copy.wait_send()
    square_copy.wait_send()


def body(
    tokens, in_gain, w_query, w_forget, w_value, w_outgate, floor_gap, extra_decay, out_gain, w_output
):
    half, width = tokens.shape
    rows = 2 * half
    chans = floor_gap.shape[0]
    heads = chans // HEAD
    chunks = rows // CHUNK
    vmem, sem = pltpu.VMEM, pltpu.SemaphoreType.DMA
    inner = pl.BlockSpec(memory_space=pltpu.VMEM)
    outer = pl.BlockSpec(memory_space=pltpu.HBM)
    square = (heads, HEAD, HEAD)
    return pl.pallas_call(
        functools.partial(kernel, lax.axis_size("sp") // 2),
        out_shape=jax.ShapeDtypeStruct((half, width), bf16),
        in_specs=[outer] * 10,
        out_specs=inner,
        scratch_shapes=[
            vmem((1, width), f32),
            vmem((1, chans), f32),
            vmem((heads, rows), f32),
            vmem((chans,), bf16),
            vmem((2, half, width), bf16),
            vmem((rows, width), bf16),
            vmem((4, width, chans), bf16),
            vmem((2, chans, width), bf16),
            vmem((4, rows, chans), bf16),
            vmem((rows, chans), f32),
            vmem((rows, chans), f32),
            vmem((chunks, heads, CHUNK), f32),
            vmem((rows, chans), bf16),
            vmem((rows, chans), bf16),
            vmem((rows, chans), f32),
            vmem((chunks,) + square, bf16),
            vmem((chunks, 1, chans), f32),
            vmem(square, f32),
            vmem((8, chans), f32),
            vmem(square, bf16),
            vmem(square, bf16),
            vmem((8, chans), f32),
            vmem(square, bf16),
            vmem(square, bf16),
            vmem(square, bf16),
            vmem((half, chans), bf16),
            vmem((half, chans), bf16),
            vmem((half, HEAD), f32),
            vmem((half, HEAD), f32),
            vmem((half, chans), bf16),
            vmem((half, width), f32),
            sem((10,)),
            sem((2,)),
            sem((2,)),
            sem((heads * PIECES + 1,)),
            sem((heads * PIECES + 1,)),
            sem((heads * PIECES,)),
            sem((heads * PIECES,)),
            sem((2,)),
            sem((2,)),
        ],
        compiler_params=pltpu.CompilerParams(
            collective_id=0, has_side_effects=True, vmem_limit_bytes=56 * 1024 * 1024
        ),
    )(
        tokens, in_gain[None, :], w_query, w_forget, w_value, w_outgate,
        floor_gap[None, :], extra_decay.T, out_gain, w_output,
    )


def solution(mesh):
    in_specs = (
        P(("grp", "sp", "tp"), None),
        P(),
        P(None, "tp"),
        P(None, "tp"),
        P(None, "tp"),
        P(None, "tp"),
        P("tp"),
        P(("grp", "sp"), "tp"),
        P("tp"),
        P("tp", None),
    )
    out_specs = P(("grp", "sp", "tp"), None)
    return jax.shard_map(body, mesh=mesh, in_specs=in_specs, out_specs=out_specs, check_vma=False)
```

```python
import functools

import jax
import jax.numpy as jnp
from jax import lax
from jax.experimental import pallas as pl
from jax.experimental.pallas import tpu as pltpu
from jax.sharding import PartitionSpec as P

HEAD = 128
CHUNK = 128
PIECES = 4
MESH = pl.DeviceIdType.MESH
epsilon = 1e-06
f32 = jnp.float32
bf16 = jnp.bfloat16


def dot(a, b):
    return jnp.dot(a, b, preferred_element_type=f32)


def dot_nt(a, b):
    return lax.dot_general(a, b, (((1,), (1,)), ((), ())), preferred_element_type=f32)


def dot_tn(a, b):
    return lax.dot_general(a, b, (((0,), (0,)), ((), ())), preferred_element_type=f32)


def split(x, parts):
    pieces = []
    for _ in range(parts):
        piece = x.astype(bf16)
        pieces.append(piece)
        x = x - piece.astype(f32)
    return pieces


def kernel(
    pairs,
    tokens, in_gain_hbm, w_query, w_forget, w_value, w_outgate, floor_hbm, extra_hbm, out_gain_hbm, w_output,
    out,
    in_gain, floor_gap, extra, out_gain, tok, normed, weights, wo, proj, cum_gate, cum_extra, extra_line, key_up, gate_factor, read_down, local_out,
    starts, offsets, own_state, own_decay, end_bf, peer_bf, peer_decay, chain_in, chain_out, incoming,
    gate_send, gate_recv, square_send, square_recv, gate_own, partial,
    load_sem, wide_send, wide_recv, state_send, state_recv, chain_send, chain_recv, last_send, last_recv,
):
    half, width = tok.shape[1], tok.shape[2]
    rows = 2 * half
    chans = floor_gap.shape[1]
    heads = chans // HEAD
    chunks = rows // CHUNK
    me = lax.axis_index("tp")
    other = 1 - me
    place = lax.axis_index("sp")
    side = place % 2
    link = place // 2
    mate = place + 1 - 2 * side

    loads = [pltpu.make_async_copy(tokens, tok.at[0], load_sem.at[0])]
    order = (w_forget, w_value, w_query, w_outgate)
    for n, w in enumerate(order):
        loads.append(pltpu.make_async_copy(w, weights.at[n], load_sem.at[1 + n]))
    loads.append(pltpu.make_async_copy(w_output, wo.at[0], load_sem.at[5]))
    small = [
        pltpu.make_async_copy(src, dst, load_sem.at[6 + n])
        for n, (src, dst) in enumerate(
            ((in_gain_hbm, in_gain), (floor_hbm, floor_gap), (extra_hbm, extra), (out_gain_hbm, out_gain))
        )
    ]
    for copy in small + loads:
        copy.start()

    barrier = pltpu.get_barrier_semaphore()
    pl.semaphore_signal(barrier, inc=1, device_id={"tp": other}, device_id_type=MESH)
    pl.semaphore_signal(barrier, inc=1, device_id={"sp": mate}, device_id_type=MESH)

    @pl.when(link > 0)
    def _():
        pl.semaphore_signal(barrier, inc=1, device_id={"sp": place - 2}, device_id_type=MESH)

    @pl.when(link < pairs - 1)
    def _():
        pl.semaphore_signal(barrier, inc=1, device_id={"sp": place + 2}, device_id_type=MESH)

    peers = 2 + jnp.minimum(link, 1) + jnp.minimum(pairs - 1 - link, 1)
    pl.semaphore_wait(barrier, peers)

    def to_tp(src, dst, send, recv):
        return pltpu.make_async_remote_copy(
            src_ref=src, dst_ref=dst, send_sem=send, recv_sem=recv,
            device_id={"tp": other}, device_id_type=MESH,
        )

    def to_sp(src, dst, send, recv, target):
        return pltpu.make_async_remote_copy(
            src_ref=src, dst_ref=dst, send_sem=send, recv_sem=recv,
            device_id={"sp": target}, device_id_type=MESH,
        )

    tok_copy = to_tp(tokens, tok.at[1], wide_send.at[0], wide_recv.at[0])
    tok_copy.start()
    wo_copy = to_tp(w_output, wo.at[1], wide_send.at[1], wide_recv.at[1])

    def normalize(slot, base):
        step = 128

        def block(n, _):
            x = tok[slot, pl.ds(pl.multiple_of(n * step, step), step), :].astype(f32)
            inv = lax.rsqrt(jnp.mean(x * x, axis=-1, keepdims=True) + epsilon)
            normed[pl.ds(pl.multiple_of(base + n * step, step), step), :] = (
                x * inv * in_gain[...]
            ).astype(bf16)
            return 0

        lax.fori_loop(0, half // step, block, 0)

    for copy in small:
        copy.wait()
    def project(n, at):
        step = 512

        def block(k, _):
            cols = pl.ds(pl.multiple_of(k * step, step), step)
            proj[n, at, cols] = dot(normed[at, :], weights[n, :, cols]).astype(bf16)
            return 0

        lax.fori_loop(0, chans // step, block, 0)

    loads[0].wait()
    normalize(0, me * half)
    near_rows = pl.ds(pl.multiple_of(me * half, half), half)
    far_rows = pl.ds(pl.multiple_of(other * half, half), half)
    every = pl.ds(0, rows)
    loads[1].wait()
    project(0, near_rows)
    tok_copy.wait_recv()
    wo_copy.start()
    normalize(1, other * half)
    project(0, far_rows)
    loads[2].wait()
    project(1, every)

    later = lax.broadcasted_iota(jnp.int32, (CHUNK, CHUNK), 0)
    sooner = lax.broadcasted_iota(jnp.int32, (CHUNK, CHUNK), 1)
    mask = later >= sooner
    lower = jnp.where(mask, 1.0, 0.0).astype(bf16)
    upper = jnp.where(later <= sooner, 1.0, 0.0).astype(bf16)

    own_state[...] = jnp.zeros_like(own_state)
    own_decay[...] = jnp.zeros_like(own_decay)

    def states(c, _):
        at = pl.ds(pl.multiple_of(c * CHUNK, CHUNK), CHUNK)
        key = floor_gap[...] / (1.0 + jnp.exp(proj[0, at, :].astype(f32)))
        gate = jnp.log1p(-key)
        summed = sum(dot(lower, piece) for piece in split(gate, 2))
        line = sum(dot(piece, upper) for piece in split(extra[:, at], 3))
        extra_line[c] = line
        extra_sum = jnp.concatenate(
            [jnp.broadcast_to(line[h : h + 1, :], (HEAD, CHUNK)).T for h in range(heads)], axis=1
        )
        cum_gate[at, :] = summed
        cum_extra[at, :] = extra_sum
        key_up[at, :] = (key * jnp.exp(-summed)).astype(bf16)
        both = summed + extra_sum
        last = both[CHUNK - 1 : CHUNK, :]
        kept = (key * jnp.exp(last - both)).astype(bf16)
        shrink = jnp.exp(last)
        offsets[c] = own_decay[0:1, :]
        own_decay[...] = own_decay[...] + last
        for h in range(heads):
            cols = slice(h * HEAD, (h + 1) * HEAD)
            state = own_state[h]
            starts[c, h] = state.astype(bf16)
            own_state[h] = state * shrink[:, cols] + dot_tn(proj[1, at, cols], kept[:, cols])
        return 0

    lax.fori_loop(0, chunks, states, 0)
    end_bf[...] = own_state[...].astype(bf16)

    spans = [(h, pl.ds(p * (HEAD // PIECES), HEAD // PIECES)) for h in range(heads) for p in range(PIECES)]
    count = len(spans)
    decay_copy = to_sp(own_decay, peer_decay, state_send.at[count], state_recv.at[count], mate)
    decay_copy.start()
    state_copies = []
    for n, (h, span) in enumerate(spans):
        copy = to_sp(end_bf.at[h, span], peer_bf.at[h, span], state_send.at[n], state_recv.at[n], mate)
        copy.start()
        state_copies.append(copy)

    loads[3].wait()
    project(2, every)
    loads[4].wait()
    project(3, every)

    def outputs(c, _):
        at = pl.ds(pl.multiple_of(c * CHUNK, CHUNK), CHUNK)
        query = proj[2, at, :].astype(f32)
        reading = query / (1.0 + jnp.exp(-query)) * HEAD ** (-0.5)
        extra_sum = cum_extra[at, :]
        near = reading * jnp.exp(cum_gate[at, :])
        far = near * jnp.exp(extra_sum)
        read_down[at, :] = (far * jnp.exp(offsets[c])).astype(bf16)
        near = near.astype(bf16)
        far = far.astype(bf16)
        for h in range(heads):
            cols = slice(h * HEAD, (h + 1) * HEAD)
            scores = dot_nt(near[:, cols], key_up[at, cols])
            differ = extra_sum[:, cols] - extra_line[c, h : h + 1, :]
            decay = jnp.where(mask, jnp.exp(differ), 0.0)
            local_out[at, cols] = dot((scores * decay).astype(bf16), proj[1, at, cols]) + dot_nt(
                far[:, cols], starts[c, h]
            )
        return 0

    gains = out_gain[...].astype(f32).reshape(1, chans)

    def factor(c, _):
        at = pl.ds(pl.multiple_of(c * CHUNK, CHUNK), CHUNK)
        gate = proj[3, at, :].astype(f32)
        gate_factor[at, :] = gains * (gate / (1.0 + jnp.exp(-gate)))
        return 0

    def compute_outputs():
        lax.fori_loop(0, chunks, outputs, 0)
        lax.fori_loop(0, chunks, factor, 0)

    onward = [
        to_sp(chain_out.at[h, span], chain_in.at[h, span], chain_send.at[n], chain_recv.at[n], place + 2)
        for n, (h, span) in enumerate(spans)
    ]
    second = side.astype(f32)
    first = 1.0 - second

    def relay():
        decay_copy.wait_recv()
        mine = own_decay[0:1, :]
        theirs = peer_decay[0:1, :]
        early = first * mine + second * theirs
        late = first * theirs + second * mine

        @pl.when(link == 0)
        def _():
            chain_in[...] = jnp.zeros_like(chain_in)

        for n, (h, span) in enumerate(spans):
            cols = slice(h * HEAD, (h + 1) * HEAD)
            state_copies[n].wait_recv()

            @pl.when(link > 0)
            def _():
                onward[n].wait_recv()

            own = own_state[h, span]
            peer = peer_bf[h, span].astype(f32)
            begun = first * own + second * peer
            ended = first * peer + second * own
            before = chain_in[h, span].astype(f32)
            middle = jnp.exp(early[:, cols]) * before + begun

            @pl.when(link < pairs - 1)
            def _():
                chain_out[h, span] = (jnp.exp(late[:, cols]) * middle + ended).astype(bf16)
                onward[n].start()

            incoming[h, span] = (first * before + second * middle).astype(bf16)

    front = pairs // 2

    @pl.when(link >= front)
    def _():
        compute_outputs()

    relay()

    @pl.when(link < front)
    def _():
        compute_outputs()

    def finish(base):
        at = pl.ds(pl.multiple_of(base, half), half)
        pieces = []
        squares = jnp.zeros((half, 1), f32)
        for h in range(heads):
            cols = slice(h * HEAD, (h + 1) * HEAD)
            total = local_out[at, cols] + dot_nt(read_down[at, cols], incoming[h])
            total = total.astype(bf16).astype(f32)
            squares = squares + jnp.sum(total * total, axis=-1, keepdims=True)
            pieces.append((total * gate_factor[at, cols]).astype(bf16))
        return pieces, squares

    pieces, squares = finish(other * half)
    for h in range(heads):
        gate_send[:, h * HEAD : (h + 1) * HEAD] = pieces[h]
    square_send[...] = jnp.broadcast_to(squares, square_send.shape)
    gate_copy = to_tp(gate_send, gate_recv, last_send.at[0], last_recv.at[0])
    square_copy = to_tp(square_send, square_recv, last_send.at[1], last_recv.at[1])
    gate_copy.start()
    square_copy.start()

    pieces, squares = finish(me * half)
    for h in range(heads):
        gate_own[:, h * HEAD : (h + 1) * HEAD] = pieces[h]
    tile = 1024
    loads[5].wait()

    def own_part(k, _):
        cols = pl.ds(pl.multiple_of(k * tile, tile), tile)
        partial[:, cols] = dot(gate_own[...], wo[0, :, cols])
        return 0

    lax.fori_loop(0, width // tile, own_part, 0)
    wo_copy.wait_recv()
    gate_copy.wait_recv()
    square_copy.wait_recv()
    scale = lax.rsqrt((squares + square_recv[:, 0:1]) / (2.0 * chans) + epsilon)

    def whole(k, _):
        cols = pl.ds(pl.multiple_of(k * tile, tile), tile)
        both = partial[:, cols] + dot(gate_recv[...], wo[1, :, cols])
        out[:, cols] = (both * scale).astype(bf16)
        return 0

    lax.fori_loop(0, width // tile, whole, 0)

    tok_copy.wait_send()
    wo_copy.wait_send()
    decay_copy.wait_send()
    for copy in state_copies:
        copy.wait_send()

    @pl.when(link < pairs - 1)
    def _():
        for copy in onward:
            copy.wait_send()

    gate_copy.wait_send()
    square_copy.wait_send()


def body(
    tokens, in_gain, w_query, w_forget, w_value, w_outgate, floor_gap, extra_decay, out_gain, w_output
):
    half, width = tokens.shape
    rows = 2 * half
    chans = floor_gap.shape[0]
    heads = chans // HEAD
    chunks = rows // CHUNK
    vmem, sem = pltpu.VMEM, pltpu.SemaphoreType.DMA
    inner = pl.BlockSpec(memory_space=pltpu.VMEM)
    outer = pl.BlockSpec(memory_space=pltpu.HBM)
    square = (heads, HEAD, HEAD)
    return pl.pallas_call(
        functools.partial(kernel, lax.axis_size("sp") // 2),
        out_shape=jax.ShapeDtypeStruct((half, width), bf16),
        in_specs=[outer] * 10,
        out_specs=inner,
        scratch_shapes=[
            vmem((1, width), f32),
            vmem((1, chans), f32),
            vmem((heads, rows), f32),
            vmem((chans,), bf16),
            vmem((2, half, width), bf16),
            vmem((rows, width), bf16),
            vmem((4, width, chans), bf16),
            vmem((2, chans, width), bf16),
            vmem((4, rows, chans), bf16),
            vmem((rows, chans), f32),
            vmem((rows, chans), f32),
            vmem((chunks, heads, CHUNK), f32),
            vmem((rows, chans), bf16),
            vmem((rows, chans), f32),
            vmem((rows, chans), bf16),
            vmem((rows, chans), f32),
            vmem((chunks,) + square, bf16),
            vmem((chunks, 1, chans), f32),
            vmem(square, f32),
            vmem((8, chans), f32),
            vmem(square, bf16),
            vmem(square, bf16),
            vmem((8, chans), f32),
            vmem(square, bf16),
            vmem(square, bf16),
            vmem(square, bf16),
            vmem((half, chans), bf16),
            vmem((half, chans), bf16),
            vmem((half, HEAD), f32),
            vmem((half, HEAD), f32),
            vmem((half, chans), bf16),
            vmem((half, width), f32),
            sem((10,)),
            sem((2,)),
            sem((2,)),
            sem((heads * PIECES + 1,)),
            sem((heads * PIECES + 1,)),
            sem((heads * PIECES,)),
            sem((heads * PIECES,)),
            sem((2,)),
            sem((2,)),
        ],
        compiler_params=pltpu.CompilerParams(
            collective_id=0, has_side_effects=True, vmem_limit_bytes=58720256
        ),
    )(
        tokens, in_gain[None, :], w_query, w_forget, w_value, w_outgate,
        floor_gap[None, :], extra_decay.T, out_gain, w_output,
    )


def solution(mesh):
    in_specs = (
        P(("grp", "sp", "tp"), None),
        P(),
        P(None, "tp"),
        P(None, "tp"),
        P(None, "tp"),
        P(None, "tp"),
        P("tp"),
        P(("grp", "sp"), "tp"),
        P("tp"),
        P("tp", None),
    )
    out_specs = P(("grp", "sp", "tp"), None)
    return jax.shard_map(body, mesh=mesh, in_specs=in_specs, out_specs=out_specs, check_vma=False)
```
